256 devices in a mesh: fs: 64 (over z, x, core), tp: 4 (over y).
Axes of the slice: x: 4, y: 4, z: 8, core: 2. Of those that a mesh axis runs over, the one named last changes fastest.
Arguments:
- tokens: bfloat16 [65536, 2048], P('fs', 'tp'), may hold values from -50 to 50
- norm_gain: float32 [2048], P('fs'), may hold values from 0.1 to 1.9
- gate_weight: float32 [2048, 2816], P('fs', 'tp'), may hold values from -0.125 to 0.125
- up_weight: float32 [2048, 2816], P('fs', 'tp'), may hold values from -0.125 to 0.125
- down_weight: float32 [2816, 2048], P('fs', 'tp'), may hold values from -0.109375 to 0.109375
Outputs:
- gate_sampler: bfloat16 [2048, 2816], P(None, 'tp')
- up_sampler: bfloat16 [2048, 2816], P(None, 'tp')
- down_sampler: bfloat16 [2816, 2048], P('tp')
- mixed: bfloat16 [65536, 2048], P('fs', 'tp')
The draws below stay inside these ranges and needn't reach their ends.
All inputs are finite; a program needn't handle non-finite values.
Results may differ from the reference program's by a relative error of at most 0.0095.
Values may be sent and summed in bfloat16 or wider, within the bound.
No kernel may reach another device: no remote copies, remote signals or barrier semaphores. Data moves between devices by JAX's collectives and lax.ppermute only.
A program may use at most 128 MiB of HBM per device.

```python
import math
import jax
import jax.numpy as jnp
from jax import lax

D = 2048
FF = 2816
TOKENS = 65536
HID_DEV = 704
N_TP = 4


def draw_tokens(key, part):
    first, second, third = jax.random.split(key, 3)
    row_scale = jnp.exp(jax.random.uniform(first, (TOKENS, 1), jnp.float32, 0.0, math.log(10.0)))
    col_scale = jnp.exp(jax.random.uniform(second, (1, D), jnp.float32, 0.0, math.log(10.0)))
    base = jnp.clip(jax.random.normal(third, (TOKENS, D), jnp.float32), -5.0, 5.0)
    return (base * row_scale * col_scale / 10.0).astype(jnp.bfloat16)


def steps_of(key, shape, cuts, low, high):
    gain, own = 1.0, jax.random.fold_in(key, 6)
    for axis_at, shards_of in cuts:
        steps = jnp.exp(jax.random.uniform(jax.random.fold_in(own, axis_at), (shards_of,), jnp.float32, low / len(cuts), high / len(cuts)))
        gain = gain * jnp.repeat(steps, shape[axis_at] // shards_of).reshape([-1 if axis == axis_at else 1 for axis in range(len(shape))])
    return gain


def gaussian(rng, shape, scale, limit, cuts=(), held_as=jnp.bfloat16):
    factor_of = steps_of(rng, shape, cuts, -0.22, 0.18) if cuts else 1.0
    values = jax.random.normal(rng, shape, jnp.float32) * scale * factor_of
    return jnp.minimum(jnp.maximum(values, -limit), limit).astype(held_as)


def setup_inputs(seed: int = 0) -> dict:
    key_of = jax.random.split(jax.random.key(seed), 6)
    return {
        "tokens": draw_tokens(jax.random.fold_in(key_of[5], 71), 0),
        "norm_gain": jnp.clip(1.0 + 0.18 * jax.random.normal(key_of[1], (D,), jnp.float32), 0.1, 1.9),
        "gate_weight": gaussian(key_of[2], (D, FF), D ** -0.5, 0.125, ((0, 64), (1, 4)), jnp.float32),
        "up_weight": gaussian(key_of[3], (D, FF), D ** -0.5, 0.125, ((0, 64), (1, 4)), jnp.float32),
        "down_weight": gaussian(key_of[4], (FF, D), FF ** -0.5, 0.109375, ((0, 64), (1, 4)), jnp.float32),
    }


norm_eps = 1e-06

def reference(tokens, norm_gain, gate_weight, up_weight, down_weight):
    gate_sampler = (norm_gain[:, None] * gate_weight).astype(jnp.bfloat16)
    up_sampler = (norm_gain[:, None] * up_weight).astype(jnp.bfloat16)
    down_sampler = down_weight.astype(jnp.bfloat16)
    floated = tokens.astype(jnp.float32)
    normed = (floated * lax.rsqrt(lax.optimization_barrier(jnp.mean(floated * floated, axis=-1, keepdims=True)) + norm_eps)).astype(jnp.bfloat16)
    gate = jnp.dot(normed, gate_sampler, preferred_element_type=jnp.float32)
    up = jnp.dot(normed, up_sampler, preferred_element_type=jnp.float32)
    hidden = (jax.nn.silu(gate) * up).astype(jnp.bfloat16)
    summed = jnp.zeros((tokens.shape[0], tokens.shape[1]), jnp.float32)
    for block_index in range(N_TP):
        low = block_index * HID_DEV
        partial_value = jnp.dot(hidden[:, low:low + HID_DEV], down_sampler[low:low + HID_DEV, :], preferred_element_type=jnp.float32).astype(jnp.bfloat16)
        partial_value = lax.optimization_barrier(partial_value)
        summed = summed + partial_value.astype(jnp.float32)
    return (gate_sampler, up_sampler, down_sampler, summed.astype(jnp.bfloat16))
```

```python
import jax
import jax.numpy as jnp
from jax import lax
from jax.sharding import Mesh
from jax.sharding import PartitionSpec as P

FS = ("z", "x", "c")

norm_eps = 1e-06


def shift(array, axis, by):
    size = lax.axis_size(axis)
    return lax.ppermute(array, axis, [(i, (i + by) % size) for i in range(size)])


def placed(blocks, axis):
    size = len(blocks)
    twice = jnp.stack(blocks + blocks[:-1])
    return lax.dynamic_slice_in_dim(twice, (size - lax.axis_index(axis)) % size, size, 0)


def ring_of_8(array, axis):
    return placed([array] + [shift(array, axis, -k) for k in range(1, 8)], axis)


def ring_of_4(array, axis):
    return placed([array] + [shift(array, axis, -k) for k in range(1, 4)], axis)


def ring_of_4_relayed(array, axis):
    half = array.shape[0] // 2
    parts = (array[:half], array[half:])
    before = [shift(p, axis, 1) for p in parts]
    after = [shift(p, axis, -1) for p in reversed(parts)][::-1]
    far = [shift(before[0], axis, 1), shift(after[1], axis, -1)]
    return [array] + [jnp.concatenate(p) for p in (after, far, before)]


def shards(tokens, norm_gain, gate_weight, up_weight, down_weight):
    y = lax.axis_index("tp")
    gain = norm_gain[:, None]
    gate_up = jnp.concatenate([gain * gate_weight, gain * up_weight], axis=1).astype(jnp.bfloat16)
    down = down_weight.astype(jnp.bfloat16)

    blocks = ring_of_4_relayed(tokens, "tp")

    by_z = ring_of_8(gate_up, "z")
    by_x = ring_of_4_relayed(by_z, "x")
    other = [lax.ppermute(b, "c", [(0, 1), (1, 0)]) for b in by_x]
    c, x = lax.axis_index("c"), lax.axis_index("x")
    both = jnp.zeros((8, 4, 2, *gate_up.shape), jnp.bfloat16)
    for k in range(4):
        both = lax.dynamic_update_slice(both, by_x[k][:, None, None], (0, (x + k) % 4, c, 0, 0))
        both = lax.dynamic_update_slice(both, other[k][:, None, None], (0, (x + k) % 4, 1 - c, 0, 0))
    both = both.reshape(2048, 1408)

    swap = [(z * 4 + t, (2 * t + z % 2) * 4 + z // 2) for z in range(8) for t in range(4)]
    down = lax.ppermute(down, ("z", "tp"), swap)
    down = ring_of_8(ring_of_4(down, "x"), "z")
    down_other = lax.ppermute(down, "c", [(0, 1), (1, 0)])
    first = jnp.where(c == 0, down, down_other)
    second = jnp.where(c == 0, down_other, down)
    down = jnp.stack([first, second], axis=2)
    down = down.reshape(4, 2, 4, 2, 44, 512)
    down_sampler = down.transpose(1, 2, 3, 4, 0, 5).reshape(704, 2048)

    squares = sum(jnp.sum(jnp.square(b.astype(jnp.float32)), axis=1, keepdims=True) for b in blocks)
    scale = lax.rsqrt(squares / 2048 + norm_eps)
    acc = 0
    for k, block in enumerate(blocks):
        rows = lax.dynamic_slice_in_dim(both, (y + k) % 4 * 512, 512, 0)
        acc = acc + jnp.dot(block, rows, preferred_element_type=jnp.float32)
    acc = acc * scale
    gate, up = acc[:, :704], acc[:, 704:]
    hidden = (jax.nn.silu(gate) * up).astype(jnp.bfloat16)

    def terms(k):
        columns = lax.dynamic_slice_in_dim(down_sampler, (y + k) % 4 * 512, 512, 1)
        return jnp.dot(hidden, columns, preferred_element_type=jnp.float32)

    h = 512
    far = terms(2).astype(jnp.bfloat16)
    from_before = shift(far[:h], "tp", 1)
    from_after = shift(far[h:], "tp", -1)
    right, left = terms(1), terms(3)
    right_low = shift(right[h:].astype(jnp.bfloat16), "tp", 1)
    left_top = shift(left[:h].astype(jnp.bfloat16), "tp", -1)
    right_top = shift((right[:h] + from_before.astype(jnp.float32)).astype(jnp.bfloat16), "tp", 1)
    left_low = shift((left[h:] + from_after.astype(jnp.float32)).astype(jnp.bfloat16), "tp", -1)
    own = terms(0)
    top = own[:h] + right_top.astype(jnp.float32) + left_top.astype(jnp.float32)
    low = own[h:] + right_low.astype(jnp.float32) + left_low.astype(jnp.float32)
    mixed = jnp.concatenate([top, low]).astype(jnp.bfloat16)
    return (both[:, :704], both[:, 704:], down_sampler, mixed)


def solution(mesh):
    finer = Mesh(mesh.devices.reshape(8, 4, 2, mesh.shape["tp"]), ("z", "x", "c", "tp"))
    return jax.shard_map(
        shards,
        mesh=finer,
        in_specs=(P(FS, "tp"), P(FS), P(FS, "tp"), P(FS, "tp"), P(FS, "tp")),
        out_specs=(P(None, "tp"), P(None, "tp"), P("tp", None), P(FS, "tp")),
        check_vma=False,
    )
```
